32 devices in a mesh: ep: 16 (over z, y, x), tp: 2 (over core).
Axes of the slice: x: 2, y: 2, z: 4, core: 2. Of those that a mesh axis runs over, the one named last changes fastest.
Arguments:
- hidden: bfloat16 [256, 2048], P('ep'), may hold values from -6 to 6
- attn_gain: bfloat16 [2048], replicated, may hold values from 0.099609375 to 1.8984375
- query_weight: bfloat16 [2048, 2048], P(None, 'tp'), may hold values from -0.125 to 0.125
- key_weight: bfloat16 [2048, 128], P(None, 'tp'), may hold values from -0.125 to 0.125
- value_weight: bfloat16 [2048, 128], P(None, 'tp'), may hold values from -0.125 to 0.125
- forget_weight: bfloat16 [2048, 32], P(None, 'tp'), may hold values from -0.125 to 0.125
- forget_bias: float32 [32], P('tp'), may hold values from -1 to 4
- cache_keys: bfloat16 [256, 2, 64, 1024], P('ep', 'tp'), may hold values from -64 to 64
- cache_values: bfloat16 [256, 2, 64, 1024], P('ep', 'tp'), may hold values from -6 to 6
- cache_logsum: float32 [256, 32, 1024], P('ep', 'tp'), may hold values from -144 to 0, as said below
- lengths: int32 [256], P('ep'), may hold values from 2 to 1023, as said below
- out_weight: bfloat16 [2048, 2048], P('ep'), may hold values from -0.125 to 0.125
- ffn_gain: bfloat16 [2048], replicated, may hold values from 0.099609375 to 1.8984375
- expert_ids: int32 [256, 6], P('ep'), may hold values from 0 to 15, all different within a row; in each aligned block of 16 rows (0 to 15, 16 to 31, ...) at most 12 rows name the same one
- expert_scores: float32 [256, 6], P('ep'), may hold values from 0.1 to 1
- gate_weights: bfloat16 [16, 2048, 512], P('ep', None, 'tp'), may hold values from -0.125 to 0.125
- up_weights: bfloat16 [16, 2048, 512], P('ep', None, 'tp'), may hold values from -0.125 to 0.125
- down_weights: bfloat16 [16, 512, 2048], P('ep', 'tp'), may hold values from -0.25 to 0.25
Outputs:
- updated: bfloat16 [256, 2048], P('ep')
- new_key: bfloat16 [256, 2, 64], P('ep', 'tp')
- new_value: bfloat16 [256, 2, 64], P('ep', 'tp')
- new_logsum: float32 [256, 32], P('ep', 'tp')
The draws below stay inside these ranges and needn't reach their ends.
Inputs may be any that keep to these rules, and one draw needn't show every extreme that they name: `cache_logsum`: non-increasing along the positions. The new token stands at position lengths; some sequence has 1023 cached positions. `expert_ids`: each row names 6 different experts; the rows of one index of ep name one expert at most 12 times.
All inputs are finite; a program needn't handle non-finite values.
Results may differ from the reference program's by a relative error of at most 0.006.
Values may be sent and summed in bfloat16 or wider, within the bound.
A program may use at most 64 MiB of HBM per device.

```python
import math
import jax
import jax.numpy as jnp
import numpy as np
from jax import lax

D = 2048
HEADS = 32
HD = 64
KV_HEADS = 2
DEXP = 512
TOP_K = 6
CACHE_POSITIONS = 1024
SEQ_DEV = 16
BATCH_SEQUENCES = 256
EXPERTS = 16
CAP = 12
N_EP = 16
N_TP = 2


def draw_cache_keys(key, part):
    random_subkeys = jax.random.split(key, 1)
    values_drawn = jnp.clip(jax.random.normal(random_subkeys[0], (BATCH_SEQUENCES, KV_HEADS, HD, CACHE_POSITIONS), jnp.float32), -6.0, 6.0)
    return values_drawn.astype(jnp.bfloat16)


def draw_cache_logsum(key, part):
    random_subkeys = jax.random.split(key, 7)
    head_order = jax.random.permutation(random_subkeys[0], HEADS)
    is_sluggish = head_order < HEADS // 2
    is_sluggish = is_sluggish.astype(jnp.float32)[None, :, None]
    slow_rate = jax.random.uniform(random_subkeys[1], (1, HEADS, 1), jnp.float32, 0.2, 0.8) / CACHE_POSITIONS
    fast_rate = 1.0 / jax.random.uniform(random_subkeys[2], (1, HEADS, 1), jnp.float32, 30.0, 100.0)
    decay_rate = is_sluggish * slow_rate + (1.0 - is_sluggish) * fast_rate
    sequence_factor = jnp.exp(jax.random.uniform(random_subkeys[3], (BATCH_SEQUENCES, 1, 1), jnp.float32, math.log(0.5), math.log(2.0)))
    random_wobble = jax.random.uniform(random_subkeys[4], (BATCH_SEQUENCES, HEADS, CACHE_POSITIONS), jnp.float32, 0.4, 1.6)
    spike_mask = (jax.random.uniform(random_subkeys[5], (BATCH_SEQUENCES, 1, CACHE_POSITIONS)) < 3.0 / CACHE_POSITIONS).astype(jnp.float32)
    shift_amount = jax.random.uniform(random_subkeys[6], (BATCH_SEQUENCES, HEADS, CACHE_POSITIONS), jnp.float32, 0.22, 0.69)
    step_logarithm = -(decay_rate * sequence_factor * random_wobble) - spike_mask * shift_amount * is_sluggish
    return jnp.cumsum(step_logarithm, axis=-1).astype(jnp.float32)


def draw_lengths(key, part):
    random_subkeys = jax.random.split(key, 2)
    groups = BATCH_SEQUENCES // SEQ_DEV
    device_top = jax.random.randint(random_subkeys[0], (groups, 1), CACHE_POSITIONS // 8, CACHE_POSITIONS - 1)
    raw_bits = jax.random.randint(random_subkeys[1], (groups, SEQ_DEV), 0, 1 << 20)
    lengths_drawn = 2 + raw_bits % (device_top - 1)
    lengths_drawn = lengths_drawn.reshape(BATCH_SEQUENCES).at[0].set(CACHE_POSITIONS - 1)
    return lengths_drawn.astype(jnp.int32)


def levels(own_key, dims, pieces, smallest, high):
    level, own = 1.0, jax.random.fold_in(own_key, 6)
    for position, blocks in pieces:
        steps = jnp.exp(jax.random.uniform(jax.random.fold_in(own, position), (blocks,), jnp.float32, smallest / len(pieces), high / len(pieces)))
        level = level * jnp.repeat(steps, dims[position] // blocks).reshape([-1 if axis == position else 1 for axis in range(len(dims))])
    return level


def deal_out(key, own, number, rows, number_of, top, most, lean):
    sequence = jax.random.permutation(key, number_of)
    packed, ordinary = load_shares(number_of, rows * top, most, lean, True), load_shares(number_of, rows * top, most, lean, False)
    places = jnp.arange(number_of)

    def named(tallies, turn):
        used = int((tallies > 0).sum())
        fixed = max(1, used // 4)
        moved = fixed + (places - fixed + turn * (used - fixed)) % max(1, number_of - fixed)
        return jnp.zeros((number_of,), jnp.int32).at[sequence[jnp.where(places < fixed, places, moved)]].set(jnp.asarray(tallies, jnp.int32))

    tallies = jnp.where(number % 4 == 0, named(packed, number // 4), named(ordinary, number - number // 4 - 1))
    mixed = jax.random.permutation(jax.random.fold_in(own, 3), number_of)
    donor, receiver = mixed[0:number_of // 2 * 2:2], mixed[1:number_of // 2 * 2:2]
    room = jnp.minimum(tallies[donor] - 1, most - tallies[receiver]) // 2
    room = jnp.where((donor == sequence[0]) | (receiver == sequence[0]) | (tallies[receiver] == 0), 0, jnp.maximum(room, 0))
    moved = jax.random.randint(jax.random.fold_in(own, 4), (number_of // 2,), 0, 1 << 20) % (room + 1)
    tallies = tallies.at[donor].add(-moved).at[receiver].add(moved)
    items = jnp.searchsorted(jnp.cumsum(tallies), jnp.arange(rows * top), side="right").astype(jnp.int32)
    listing = items.reshape(top, rows).T
    listing = listing[jax.random.permutation(jax.random.fold_in(own, 1), rows)]
    turn = jax.random.randint(jax.random.fold_in(own, 2), (rows, 1), 0, top)
    return jnp.take_along_axis(listing, (jnp.arange(top)[None, :] + turn) % top, axis=1)


def load_shares(amount, total, reach, skew, full):
    portions = [(1 << 20) // math.isqrt(standing ** skew) + 1 for standing in range(1, amount + 1)]
    largest = reach if full else min(reach, max(-(-total // amount), total * portions[0] // sum(portions)))
    least = 1 if total - largest >= amount - 1 else 0
    given, rest = [largest] + [least] * (amount - 1), total - largest - least * (amount - 1)
    while rest > 0:
        movable = [i for i in range(1, amount) if given[i] < largest] or [i for i in range(1, amount) if given[i] < reach]
        whole, remaining = sum([portions[i] for i in movable]), rest
        for i in movable:
            more = min(reach - given[i], max(1, remaining * portions[i] // whole), rest)
            given[i] = given[i] + more
            rest = rest - more
    return np.array(given)


def bell_draw(stream_key, dims, spread, reach, cuts=(), kind=jnp.bfloat16):
    values = jax.random.normal(stream_key, dims, jnp.float32) * spread
    if len(cuts) > 0:
        values = levels(stream_key, dims, cuts, -0.22, 0.18) * values
    return jnp.clip(values, min=-reach, max=reach).astype(kind)


def setup_inputs(seed: int = 0) -> dict:
    arg_keys = jax.random.split(jax.random.key(seed), 19)
    hidden = bell_draw(arg_keys[0], (BATCH_SEQUENCES, D), 1.0, 6.0, ((0, 16),))
    attn_gain = jnp.clip(1.0 + 0.18 * jax.random.normal(arg_keys[1], (D,), jnp.float32), 0.099609375, 1.8984375).astype(jnp.bfloat16)
    query_weight = bell_draw(arg_keys[2], (D, HEADS * HD), D ** -0.5, 0.125, ((1, 2),))
    key_weight = bell_draw(arg_keys[3], (D, KV_HEADS * HD), D ** -0.5, 0.125, ((1, 2),))
    value_weight = bell_draw(arg_keys[4], (D, KV_HEADS * HD), D ** -0.5, 0.125, ((1, 2),))
    forget_weight = bell_draw(arg_keys[5], (D, HEADS), D ** -0.5, 0.125, ((1, 2),))
    forget_bias = jnp.clip(-1.0 + 5.0 * jax.random.uniform(arg_keys[6], (HEADS,), jnp.float32) ** levels(arg_keys[6], (HEADS,), ((0, 2),), -0.2, 0.2), -1.0, 4.0)
    cache_keys = draw_cache_keys(jax.random.fold_in(arg_keys[18], 71), 0)
    cache_values = bell_draw(arg_keys[8], (BATCH_SEQUENCES, KV_HEADS, HD, CACHE_POSITIONS), 1.0, 6.0, ((0, 16), (1, 2)))
    cache_logsum = draw_cache_logsum(jax.random.fold_in(arg_keys[18], 71), 0)
    lengths = draw_lengths(jax.random.fold_in(arg_keys[18], 71), 0)
    out_weight = bell_draw(arg_keys[11], (D, HEADS * HD), (HEADS * HD) ** -0.5, 0.125, ((0, 16),))
    ffn_gain = jnp.clip(1.0 + 0.18 * jax.random.normal(arg_keys[12], (D,), jnp.float32), 0.099609375, 1.8984375).astype(jnp.bfloat16)
    expert_ids_keys = jax.random.split(jax.random.fold_in(arg_keys[13], 1), BATCH_SEQUENCES // SEQ_DEV)
    expert_ids_turns = jax.random.permutation(jax.random.fold_in(arg_keys[13], 3), BATCH_SEQUENCES // SEQ_DEV)
    expert_ids = jax.vmap(lambda own, number: deal_out(jax.random.fold_in(arg_keys[13], 2), own, number, SEQ_DEV, EXPERTS, TOP_K, CAP, 2))(expert_ids_keys, expert_ids_turns).reshape((BATCH_SEQUENCES, TOP_K))
    expert_scores = jnp.clip(jnp.exp(math.log(1.0) - 2.3025851 * jax.random.uniform(arg_keys[14], (BATCH_SEQUENCES, TOP_K), jnp.float32) ** levels(arg_keys[14], (BATCH_SEQUENCES, TOP_K), ((0, 16),), -0.2, 0.2)), 0.1, 1.0)
    gate_weights = bell_draw(arg_keys[15], (EXPERTS, D, DEXP), D ** -0.5, 0.125, ((0, 16), (2, 2)))
    up_weights = bell_draw(arg_keys[16], (EXPERTS, D, DEXP), D ** -0.5, 0.125, ((0, 16), (2, 2)))
    down_weights = bell_draw(arg_keys[17], (EXPERTS, DEXP, D), DEXP ** -0.5, 0.25, ((0, 16), (1, 2)))
    return {"hidden": hidden, "attn_gain": attn_gain, "query_weight": query_weight, "key_weight": key_weight, "value_weight": value_weight, "forget_weight": forget_weight, "forget_bias": forget_bias, "cache_keys": cache_keys, "cache_values": cache_values, "cache_logsum": cache_logsum, "lengths": lengths, "out_weight": out_weight, "ffn_gain": ffn_gain, "expert_ids": expert_ids, "expert_scores": expert_scores, "gate_weights": gate_weights, "up_weights": up_weights, "down_weights": down_weights}


epsilon = 1e-06

def root_norm(values_in, gain):
    floats = values_in.astype(jnp.float32)
    inv_root = lax.rsqrt(lax.optimization_barrier(jnp.mean(floats * floats, axis=-1, keepdims=True)) + epsilon)
    return floats * inv_root * gain.astype(jnp.float32)

def attend(block):
    queries, keys_block, values_block, logsum_block, lengths_block, key_new, value_new, newsum = block
    rows_here = queries.shape[0]
    query_heads = queries.shape[1] // HD
    key_heads = keys_block.shape[1]
    group_size = query_heads // key_heads
    score_scale = HD ** (-0.5)
    grouped = queries.astype(jnp.float32).reshape(rows_here, key_heads, group_size, HD)
    scores = jnp.einsum('sgjd,sgdp->sgjp', grouped, keys_block.astype(jnp.float32))
    scores = scores.reshape(rows_here, query_heads, CACHE_POSITIONS) * score_scale
    scores = scores + newsum[:, :, None] - logsum_block
    positions = jnp.arange(CACHE_POSITIONS, dtype=jnp.int32)
    is_live = positions[None, :] < lengths_block[:, None]
    scores = jnp.where(is_live[:, None, :], scores, -jnp.inf)
    own_score = jnp.einsum('sgjd,sgd->sgj', grouped, key_new.astype(jnp.float32)).reshape(rows_here, query_heads) * score_scale
    top_score = jnp.maximum(lax.optimization_barrier(jnp.max(scores, axis=-1)), own_score)
    past_exp = jnp.exp(scores - top_score[:, :, None])
    own_exp = jnp.exp(own_score - top_score)
    denominator = lax.optimization_barrier(jnp.sum(past_exp, axis=-1)) + own_exp
    past_weight = (past_exp / denominator[:, :, None]).astype(jnp.bfloat16)
    own_weight = (own_exp / denominator).astype(jnp.bfloat16)
    attended = jnp.einsum('sgjp,sgdp->sgjd', past_weight.astype(jnp.float32).reshape(rows_here, key_heads, group_size, CACHE_POSITIONS), values_block.astype(jnp.float32))
    attended = attended + own_weight.astype(jnp.float32).reshape(rows_here, key_heads, group_size)[:, :, :, None] * value_new.astype(jnp.float32)[:, :, None, :]
    return attended.reshape(rows_here, query_heads * HD).astype(jnp.bfloat16)

def blocked(array):
    return array.reshape((BATCH_SEQUENCES // SEQ_DEV, SEQ_DEV) + array.shape[1:])

def reference(hidden, attn_gain, query_weight, key_weight, value_weight, forget_weight, forget_bias, cache_keys, cache_values, cache_logsum, lengths, out_weight, ffn_gain, expert_ids, expert_scores, gate_weights, up_weights, down_weights):
    normed = root_norm(hidden, attn_gain).astype(jnp.bfloat16)
    queries = jnp.dot(normed, query_weight, preferred_element_type=jnp.float32).astype(jnp.bfloat16)
    new_key = jnp.dot(normed, key_weight, preferred_element_type=jnp.float32).astype(jnp.bfloat16).reshape(BATCH_SEQUENCES, KV_HEADS, HD)
    new_value = jnp.dot(normed, value_weight, preferred_element_type=jnp.float32).astype(jnp.bfloat16).reshape(BATCH_SEQUENCES, KV_HEADS, HD)
    log_forget = jax.nn.log_sigmoid(jnp.dot(normed, forget_weight, preferred_element_type=jnp.float32) + forget_bias)
    positions = jnp.arange(CACHE_POSITIONS, dtype=jnp.int32)
    is_last = positions[None, :] == (lengths - 1)[:, None]
    new_logsum = lax.optimization_barrier(jnp.sum(jnp.where(is_last[:, None, :], cache_logsum, 0.0), axis=-1)) + log_forget
    blocks = tuple((blocked(array) for array in (queries, cache_keys, cache_values, cache_logsum, lengths, new_key, new_value, new_logsum)))
    attended = lax.map(attend, blocks).reshape(BATCH_SEQUENCES, HEADS * HD)
    mixed = jnp.dot(attended, out_weight.T, preferred_element_type=jnp.float32).astype(jnp.bfloat16)
    residual = hidden.astype(jnp.float32) + mixed.astype(jnp.float32)
    ffn_in = root_norm(residual, ffn_gain).astype(jnp.bfloat16)
    route_count = BATCH_SEQUENCES * TOP_K
    flat_ids = expert_ids.reshape(route_count)
    onehot = (flat_ids[:, None] == jnp.arange(EXPERTS, dtype=jnp.int32)[None, :]).astype(jnp.int32)
    running = jnp.cumsum(onehot.reshape(N_EP, SEQ_DEV * TOP_K, EXPERTS), axis=1).reshape(route_count, EXPERTS)
    slot_index = lax.optimization_barrier(jnp.sum(running * onehot, axis=1)) - 1
    source = jnp.arange(route_count, dtype=jnp.int32) // (SEQ_DEV * TOP_K)
    placement = flat_ids * (N_EP * CAP) + source * CAP + slot_index
    token_of_route = jnp.arange(route_count, dtype=jnp.int32) // TOP_K
    slot_table = jnp.full((EXPERTS * N_EP * CAP,), BATCH_SEQUENCES, dtype=jnp.int32).at[placement].set(token_of_route)
    padded = jnp.concatenate([ffn_in, jnp.zeros((1, D), jnp.bfloat16)], axis=0)
    expert_rows = padded[slot_table].reshape(EXPERTS, N_EP * CAP, D)
    share_width = DEXP // N_TP

    def run_expert(block):
        rows_in, gate_one, up_one, down_one = block
        gate_act = jnp.dot(rows_in, gate_one, preferred_element_type=jnp.float32)
        up_act = jnp.dot(rows_in, up_one, preferred_element_type=jnp.float32)
        hidden_act = (jax.nn.silu(gate_act) * up_act).astype(jnp.bfloat16)
        summed = jnp.zeros((rows_in.shape[0], D), jnp.float32)
        for block_index in range(N_TP):
            lower = block_index * share_width
            partial_value = jnp.dot(hidden_act[:, lower:lower + share_width], down_one[lower:lower + share_width], preferred_element_type=jnp.float32)
            summed = summed + partial_value.astype(jnp.bfloat16).astype(jnp.float32)
        return summed.astype(jnp.bfloat16)
    expert_outputs = lax.map(run_expert, (expert_rows, gate_weights, up_weights, down_weights))
    route_out = expert_outputs.reshape(EXPERTS * N_EP * CAP, D)[placement].astype(jnp.float32).reshape(BATCH_SEQUENCES, TOP_K, D)
    route_weight = expert_scores / lax.optimization_barrier(jnp.sum(expert_scores, axis=-1, keepdims=True))
    updated = (residual + lax.optimization_barrier(jnp.sum(route_out * route_weight[:, :, None], axis=1))).astype(jnp.bfloat16)
    return (updated, new_key, new_value, new_logsum)
```

```python
import functools

import jax
import jax.numpy as jnp
from jax import lax
from jax.experimental import pallas as pl
from jax.experimental.pallas import tpu as pltpu
from jax.sharding import PartitionSpec as P

HD = 64
TOP_K = 6


epsilon = 1e-06


def root_norm(values_in, gain):
    floats = values_in.astype(jnp.float32)
    inv_root = lax.rsqrt(jnp.mean(floats * floats, axis=-1, keepdims=True) + epsilon)
    return floats * inv_root * gain.astype(jnp.float32)


def attend(hidden, attn_gain, query_weight, key_weight, value_weight, forget_weight, forget_bias,
           cache_keys, cache_values, cache_logsum, lengths):
    rows_here = hidden.shape[0]
    query_heads = query_weight.shape[1] // HD
    key_heads = key_weight.shape[1] // HD
    group_size = query_heads // key_heads
    cache_len = cache_keys.shape[-1]
    score_scale = HD ** (-0.5)
    normed = root_norm(hidden, attn_gain).astype(jnp.bfloat16)
    queries = jnp.dot(normed, query_weight, preferred_element_type=jnp.float32).astype(jnp.bfloat16)
    key_new = (
        jnp.dot(normed, key_weight, preferred_element_type=jnp.float32)
        .astype(jnp.bfloat16)
        .reshape(rows_here, key_heads, HD)
    )
    value_new = (
        jnp.dot(normed, value_weight, preferred_element_type=jnp.float32)
        .astype(jnp.bfloat16)
        .reshape(rows_here, key_heads, HD)
    )
    log_forget = jax.nn.log_sigmoid(
        jnp.dot(normed, forget_weight, preferred_element_type=jnp.float32) + forget_bias
    )
    positions = jnp.arange(cache_len, dtype=jnp.int32)
    is_last = positions[None, :] == (lengths - 1)[:, None]
    new_logsum = jnp.sum(jnp.where(is_last[:, None, :], cache_logsum, 0.0), axis=-1) + log_forget
    grouped = queries.reshape(rows_here, key_heads, group_size, HD)
    scores = jnp.einsum("sgjd,sgdp->sgjp", grouped, cache_keys, preferred_element_type=jnp.float32)
    scores = scores.reshape(rows_here, query_heads, cache_len) * score_scale
    scores = scores + new_logsum[:, :, None] - cache_logsum
    is_live = positions[None, :] < lengths[:, None]
    scores = jnp.where(is_live[:, None, :], scores, -jnp.inf)
    own_score = (
        jnp.einsum("sgjd,sgd->sgj", grouped, key_new, preferred_element_type=jnp.float32).reshape(
            rows_here, query_heads
        )
        * score_scale
    )
    top_score = jnp.maximum(jnp.max(scores, axis=-1), own_score)
    past_exp = jnp.exp(scores - top_score[:, :, None])
    own_exp = jnp.exp(own_score - top_score)
    denominator = jnp.sum(past_exp, axis=-1) + own_exp
    past_weight = (past_exp / denominator[:, :, None]).astype(jnp.bfloat16)
    own_weight = (own_exp / denominator).astype(jnp.bfloat16)
    attended = jnp.einsum(
        "sgjp,sgdp->sgjd",
        past_weight.reshape(rows_here, key_heads, group_size, cache_len),
        cache_values,
        preferred_element_type=jnp.float32,
    )
    attended = (
        attended
        + own_weight.astype(jnp.float32).reshape(rows_here, key_heads, group_size)[:, :, :, None]
        * value_new.astype(jnp.float32)[:, :, None, :]
    )
    attended = attended.reshape(rows_here, query_heads * HD).astype(jnp.bfloat16)
    return attended, key_new, value_new, new_logsum


def rest_general(attended, hidden, out_weight, ffn_gain, expert_ids, expert_scores,
                 gate_weights, up_weights, down_weights):
    rows_here = hidden.shape[0]
    whole_heads = lax.all_gather(attended, "tp", axis=1, tiled=True)
    projected = lax.dot_general(
        lax.all_gather(whole_heads, "ep", axis=0, tiled=True),
        out_weight,
        (((1,), (1,)), ((), ())),
        preferred_element_type=jnp.float32,
    ).astype(jnp.bfloat16)
    mixed = lax.all_to_all(projected, "ep", split_axis=0, concat_axis=1, tiled=True)
    residual = hidden.astype(jnp.float32) + mixed.astype(jnp.float32)
    ffn_in = root_norm(residual, ffn_gain).astype(jnp.bfloat16)
    ep_size = lax.axis_size("ep")
    local_experts = gate_weights.shape[0]
    experts = ep_size * local_experts
    route_count = rows_here * TOP_K
    capacity = 2 * ((route_count + experts - 1) // experts)
    flat_ids = expert_ids.reshape(route_count)
    onehot = (flat_ids[:, None] == jnp.arange(experts, dtype=jnp.int32)[None, :]).astype(jnp.int32)
    running = jnp.cumsum(onehot, axis=0)
    slot_index = jnp.sum(running * onehot, axis=1) - 1
    target = flat_ids * capacity + slot_index
    dispatch_map = (
        target[:, None] == jnp.arange(experts * capacity, dtype=jnp.int32)[None, :]
    ).astype(jnp.bfloat16)
    route_rows = jnp.repeat(ffn_in, TOP_K, axis=0)
    outgoing = lax.dot_general(
        dispatch_map, route_rows, (((0,), (0,)), ((), ())), preferred_element_type=jnp.float32
    )
    outgoing = outgoing.astype(jnp.bfloat16).reshape(
        ep_size, local_experts, capacity, ffn_in.shape[1]
    )
    arrived = lax.all_to_all(outgoing, "ep", split_axis=0, concat_axis=0, tiled=True)
    gate_act = jnp.einsum(
        "sekd,edf->sekf", arrived, gate_weights, preferred_element_type=jnp.float32
    )
    up_act = jnp.einsum("sekd,edf->sekf", arrived, up_weights, preferred_element_type=jnp.float32)
    hidden_act = (jax.nn.silu(gate_act) * up_act).astype(jnp.bfloat16)
    partial_out = jnp.einsum(
        "sekf,efd->sekd", hidden_act, down_weights, preferred_element_type=jnp.float32
    )
    half_sum = lax.psum_scatter(
        partial_out.astype(jnp.bfloat16), "tp", scatter_dimension=3, tiled=True
    )
    sent_back = lax.all_to_all(half_sum, "ep", split_axis=0, concat_axis=0, tiled=True)
    share_width = sent_back.shape[-1]
    picked = jnp.dot(
        dispatch_map,
        sent_back.reshape(experts * capacity, share_width),
        preferred_element_type=jnp.float32,
    )
    route_weight = expert_scores / jnp.sum(expert_scores, axis=-1, keepdims=True)
    expert_mix = jnp.sum(
        picked.reshape(rows_here, TOP_K, share_width) * route_weight[:, :, None], axis=1
    )
    own_part = lax.dynamic_slice_in_dim(
        residual, lax.axis_index("tp") * share_width, share_width, 1
    )
    updated = lax.all_gather((own_part + expert_mix).astype(jnp.bfloat16), "tp", axis=1, tiled=True)
    return updated


MESH = pl.DeviceIdType.MESH


def rest_body(n, att_ref, hid_ref, gain_ref, mix_ref, ow_hbm, gate_hbm, up_hbm, down_hbm, out_ref,
              heads, ow, gate, up, down, part, part_in, proj, mixed, resid, rows, act, eout, back, upd,
              send, recv, pair_send, pair_recv, local):
    me, tp = lax.axis_index("ep"), lax.axis_index("tp")
    seqs, width = hid_ref.shape
    half = width // 2
    feats = ow.shape[0]
    cols = att_ref.shape[1]
    peers = [lax.rem(me + k, n) for k in range(1, n)]
    sources = [lax.rem(me + n - k, n) for k in range(1, n)]

    def mine(i):
        return pl.ds(pl.multiple_of(i * seqs, seqs), seqs)

    my_half = pl.ds(pl.multiple_of(tp * half, half), half)
    other_half = pl.ds(pl.multiple_of((1 - tp) * half, half), half)

    def remote(src, dst, s, r, ep, core):
        return pltpu.make_async_remote_copy(
            src_ref=src, dst_ref=dst, send_sem=s, recv_sem=r, device_id=(ep, core), device_id_type=MESH)

    loads = [
        pltpu.make_async_copy(ow_hbm.at[:, pl.ds(pl.multiple_of(tp * cols, cols), cols)], ow, local.at[0]),
        pltpu.make_async_copy(gate_hbm, gate, local.at[1]),
        pltpu.make_async_copy(up_hbm, up, local.at[2]),
        pltpu.make_async_copy(down_hbm.at[:, my_half], down.at[tp], local.at[3]),
    ]
    for c in loads:
        c.start()
    barrier = pltpu.get_barrier_semaphore()
    for p in peers:
        pl.semaphore_signal(barrier, inc=1, device_id=(p, tp), device_id_type=MESH)
    pl.semaphore_signal(barrier, inc=1, device_id=(me, 1 - tp), device_id_type=MESH)
    pl.semaphore_wait(barrier, n)

    sent = []

    def begin(c):
        c.start()
        sent.append(c)
        return c

    first = [begin(remote(att_ref, heads.at[mine(me)], send.at[0, k], recv.at[0, k], p, tp))
             for k, p in enumerate(peers)]
    swap_down = begin(remote(down_hbm.at[:, other_half], down.at[tp], pair_send.at[0], pair_recv.at[0], me, 1 - tp))
    heads[mine(me), :] = att_ref[...]
    loads[0].wait()
    for c in first:
        c.wait_recv()
    part[...] = lax.dot_general(heads[...], ow[...], (((1,), (1,)), ((), ())), preferred_element_type=jnp.float32)
    swap = begin(remote(part, part_in, pair_send.at[1], pair_recv.at[1], me, 1 - tp))
    swap.wait_recv()
    proj[...] = (part[...] + part_in[...]).astype(jnp.bfloat16)
    my_feats = pl.ds(pl.multiple_of(me * feats, feats), feats)
    second = [begin(remote(proj.at[mine(p)], mixed.at[:, my_feats], send.at[1, k], recv.at[1, k], p, tp))
              for k, p in enumerate(peers)]
    mixed[:, my_feats] = proj[mine(me), :]
    for c in second:
        c.wait_recv()
    residual = hid_ref[...].astype(jnp.float32) + mixed[...].astype(jnp.float32)
    resid[...] = residual
    rows[mine(me), :] = root_norm(residual, gain_ref[...]).astype(jnp.bfloat16)

    third = [begin(remote(rows.at[mine(me), my_half], rows.at[mine(me), my_half],
                          send.at[2, k], recv.at[2, k], p, tp)) for k, p in enumerate(peers)]
    fourth = []
    for k, s in enumerate(sources):
        third[k].wait_recv()
        fourth.append(begin(remote(rows.at[mine(s), my_half], rows.at[mine(s), my_half],
                                   send.at[3, k], recv.at[3, k], me, 1 - tp)))
    loads[1].wait()
    loads[2].wait()
    for c in fourth:
        c.wait_recv()
    gate_act = jnp.dot(rows[...], gate[...], preferred_element_type=jnp.float32)
    up_act = jnp.dot(rows[...], up[...], preferred_element_type=jnp.float32)
    act[tp] = (gate_act / (1.0 + jnp.exp(-gate_act)) * up_act).astype(jnp.bfloat16)
    swap = begin(remote(act.at[tp], act.at[tp], pair_send.at[2], pair_recv.at[2], me, 1 - tp))
    loads[3].wait()
    swap_down.wait_recv()
    swap.wait_recv()
    eout[...] = (jnp.dot(act[0], down[0], preferred_element_type=jnp.float32)
                 + jnp.dot(act[1], down[1], preferred_element_type=jnp.float32)).astype(jnp.bfloat16)
    fifth = [begin(remote(eout.at[mine(p)], back.at[me], send.at[4, k], recv.at[4, k], p, tp))
             for k, p in enumerate(peers)]
    back[me] = eout[mine(me), :]
    for c in fifth:
        c.wait_recv()
    total = resid[:, my_half]
    weights = mix_ref[...]
    summed = jnp.zeros_like(total)
    for e in range(n):
        summed = summed + weights[:, e:e + 1] * back[e].astype(jnp.float32)
    upd[:, my_half] = (total + summed).astype(jnp.bfloat16)
    swap = begin(remote(upd.at[:, my_half], upd.at[:, my_half], pair_send.at[3], pair_recv.at[3], me, 1 - tp))
    swap.wait_recv()
    out_ref[...] = upd[...]
    for c in sent:
        c.wait_send()


def rest_kernel(attended, hidden, out_weight, ffn_gain, expert_ids, expert_scores,
                gate_weights, up_weights, down_weights):
    n = lax.axis_size("ep")
    seqs, width = hidden.shape
    cols = attended.shape[1]
    feats = out_weight.shape[0]
    units = gate_weights.shape[2]
    half = width // 2
    route_weight = expert_scores / jnp.sum(expert_scores, axis=-1, keepdims=True)
    lanes = -(-n // 128) * 128
    chosen = expert_ids[:, :, None] == jnp.arange(lanes, dtype=jnp.int32)[None, None, :]
    mix = jnp.sum(jnp.where(chosen, route_weight[:, :, None], 0.0), axis=1)
    bf16, f32 = jnp.bfloat16, jnp.float32
    vmem = pl.BlockSpec(memory_space=pltpu.VMEM)
    hbm = pl.BlockSpec(memory_space=pl.ANY)
    return pl.pallas_call(
        functools.partial(rest_body, n),
        out_shape=jax.ShapeDtypeStruct((seqs, width), bf16),
        in_specs=[vmem] * 4 + [hbm] * 4,
        out_specs=vmem,
        scratch_shapes=[
            pltpu.VMEM((n * seqs, cols), bf16),
            pltpu.VMEM((feats, cols), bf16),
            pltpu.VMEM((width, units), bf16),
            pltpu.VMEM((width, units), bf16),
            pltpu.VMEM((2, units, half), bf16),
            pltpu.VMEM((n * seqs, feats), f32),
            pltpu.VMEM((n * seqs, feats), f32),
            pltpu.VMEM((n * seqs, feats), bf16),
            pltpu.VMEM((seqs, width), bf16),
            pltpu.VMEM((seqs, width), f32),
            pltpu.VMEM((n * seqs, width), bf16),
            pltpu.VMEM((2, n * seqs, units), bf16),
            pltpu.VMEM((n * seqs, half), bf16),
            pltpu.VMEM((n, seqs, half), bf16),
            pltpu.VMEM((seqs, width), bf16),
            pltpu.SemaphoreType.DMA((5, n)),
            pltpu.SemaphoreType.DMA((5, n)),
            pltpu.SemaphoreType.DMA((4,)),
            pltpu.SemaphoreType.DMA((4,)),
            pltpu.SemaphoreType.DMA((4,)),
        ],
        compiler_params=pltpu.CompilerParams(
            collective_id=0, has_side_effects=True, vmem_limit_bytes=40 * 1024 * 1024),
    )(attended, hidden, ffn_gain[None, :], mix, out_weight, gate_weights[0], up_weights[0], down_weights[0])


def per_device(
    hidden,
    attn_gain,
    query_weight,
    key_weight,
    value_weight,
    forget_weight,
    forget_bias,
    cache_keys,
    cache_values,
    cache_logsum,
    lengths,
    out_weight,
    ffn_gain,
    expert_ids,
    expert_scores,
    gate_weights,
    up_weights,
    down_weights,
):
    attended, key_new, value_new, new_logsum = attend(
        hidden, attn_gain, query_weight, key_weight, value_weight, forget_weight, forget_bias,
        cache_keys, cache_values, cache_logsum, lengths)
    rest = rest_kernel if out_weight.shape[0] % 128 == 0 and gate_weights.shape[0] == 1 else rest_general
    updated = rest(attended, hidden, out_weight, ffn_gain, expert_ids, expert_scores,
                   gate_weights, up_weights, down_weights)
    return (updated, key_new, value_new, new_logsum)


def solution(mesh):
    in_specs = (
        P("ep", None),
        P(),
        P(None, "tp"),
        P(None, "tp"),
        P(None, "tp"),
        P(None, "tp"),
        P("tp"),
        P("ep", "tp", None, None),
        P("ep", "tp", None, None),
        P("ep", "tp", None),
        P("ep"),
        P("ep", None),
        P(),
        P("ep", None),
        P("ep", None),
        P("ep", None, "tp"),
        P("ep", None, "tp"),
        P("ep", "tp", None),
    )
    out_specs = (P("ep", None), P("ep", "tp", None), P("ep", "tp", None), P("ep", "tp"))
    return jax.shard_map(
        per_device, mesh=mesh, in_specs=in_specs, out_specs=out_specs, check_vma=False
    )
```

```python
import functools
import math

import jax
import jax.numpy as jnp
from jax import lax
from jax.experimental import pallas as pl
from jax.experimental.pallas import tpu as pltpu
from jax.sharding import PartitionSpec as P

HD = 64
TOP_K = 6


epsilon = 1e-06


def root_norm(values_in, gain):
    floats = values_in.astype(jnp.float32)
    inv_root = lax.rsqrt(jnp.mean(floats * floats, axis=-1, keepdims=True) + epsilon)
    return floats * inv_root * gain.astype(jnp.float32)


def attend(hidden, attn_gain, query_weight, key_weight, value_weight, forget_weight, forget_bias,
           cache_keys, cache_values, cache_logsum, lengths):
    rows_here = hidden.shape[0]
    query_heads = query_weight.shape[1] // HD
    key_heads = key_weight.shape[1] // HD
    group_size = query_heads // key_heads
    cache_len = cache_keys.shape[-1]
    score_scale = HD ** (-0.5)
    normed = root_norm(hidden, attn_gain).astype(jnp.bfloat16)
    queries = jnp.dot(normed, query_weight, preferred_element_type=jnp.float32).astype(jnp.bfloat16)
    key_new = (
        jnp.dot(normed, key_weight, preferred_element_type=jnp.float32)
        .astype(jnp.bfloat16)
        .reshape(rows_here, key_heads, HD)
    )
    value_new = (
        jnp.dot(normed, value_weight, preferred_element_type=jnp.float32)
        .astype(jnp.bfloat16)
        .reshape(rows_here, key_heads, HD)
    )
    log_forget = jax.nn.log_sigmoid(
        jnp.dot(normed, forget_weight, preferred_element_type=jnp.float32) + forget_bias
    )
    positions = jnp.arange(cache_len, dtype=jnp.int32)
    is_last = positions[None, :] == (lengths - 1)[:, None]
    new_logsum = jnp.sum(jnp.where(is_last[:, None, :], cache_logsum, 0.0), axis=-1) + log_forget
    grouped = queries.reshape(rows_here, key_heads, group_size, HD)
    scores = jnp.einsum("sgjd,sgdp->sgjp", grouped, cache_keys, preferred_element_type=jnp.float32)
    scores = scores.reshape(rows_here, query_heads, cache_len) * score_scale
    scores = scores + new_logsum[:, :, None] - cache_logsum
    is_live = positions[None, :] < lengths[:, None]
    scores = jnp.where(is_live[:, None, :], scores, -jnp.inf)
    own_score = (
        jnp.einsum("sgjd,sgd->sgj", grouped, key_new, preferred_element_type=jnp.float32).reshape(
            rows_here, query_heads
        )
        * score_scale
    )
    top_score = jnp.maximum(jnp.max(scores, axis=-1), own_score)
    past_exp = jnp.exp(scores - top_score[:, :, None])
    own_exp = jnp.exp(own_score - top_score)
    denominator = jnp.sum(past_exp, axis=-1) + own_exp
    past_weight = (past_exp / denominator[:, :, None]).astype(jnp.bfloat16)
    own_weight = (own_exp / denominator).astype(jnp.bfloat16)
    attended = jnp.einsum(
        "sgjp,sgdp->sgjd",
        past_weight.reshape(rows_here, key_heads, group_size, cache_len),
        cache_values,
        preferred_element_type=jnp.float32,
    )
    attended = (
        attended
        + own_weight.astype(jnp.float32).reshape(rows_here, key_heads, group_size)[:, :, :, None]
        * value_new.astype(jnp.float32)[:, :, None, :]
    )
    attended = attended.reshape(rows_here, query_heads * HD).astype(jnp.bfloat16)
    return attended, key_new, value_new, new_logsum


def rest_general(attended, hidden, out_weight, ffn_gain, expert_ids, expert_scores,
                 gate_weights, up_weights, down_weights):
    rows_here = hidden.shape[0]
    whole_heads = lax.all_gather(attended, "tp", axis=1, tiled=True)
    projected = lax.dot_general(
        lax.all_gather(whole_heads, "ep", axis=0, tiled=True),
        out_weight,
        (((1,), (1,)), ((), ())),
        preferred_element_type=jnp.float32,
    ).astype(jnp.bfloat16)
    mixed = lax.all_to_all(projected, "ep", split_axis=0, concat_axis=1, tiled=True)
    residual = hidden.astype(jnp.float32) + mixed.astype(jnp.float32)
    ffn_in = root_norm(residual, ffn_gain).astype(jnp.bfloat16)
    ep_size = lax.axis_size("ep")
    local_experts = gate_weights.shape[0]
    experts = ep_size * local_experts
    route_count = rows_here * TOP_K
    capacity = 2 * ((route_count + experts - 1) // experts)
    flat_ids = expert_ids.reshape(route_count)
    onehot = (flat_ids[:, None] == jnp.arange(experts, dtype=jnp.int32)[None, :]).astype(jnp.int32)
    running = jnp.cumsum(onehot, axis=0)
    slot_index = jnp.sum(running * onehot, axis=1) - 1
    target = flat_ids * capacity + slot_index
    dispatch_map = (
        target[:, None] == jnp.arange(experts * capacity, dtype=jnp.int32)[None, :]
    ).astype(jnp.bfloat16)
    route_rows = jnp.repeat(ffn_in, TOP_K, axis=0)
    outgoing = lax.dot_general(
        dispatch_map, route_rows, (((0,), (0,)), ((), ())), preferred_element_type=jnp.float32
    )
    outgoing = outgoing.astype(jnp.bfloat16).reshape(
        ep_size, local_experts, capacity, ffn_in.shape[1]
    )
    arrived = lax.all_to_all(outgoing, "ep", split_axis=0, concat_axis=0, tiled=True)
    gate_act = jnp.einsum(
        "sekd,edf->sekf", arrived, gate_weights, preferred_element_type=jnp.float32
    )
    up_act = jnp.einsum("sekd,edf->sekf", arrived, up_weights, preferred_element_type=jnp.float32)
    hidden_act = (jax.nn.silu(gate_act) * up_act).astype(jnp.bfloat16)
    partial_out = jnp.einsum(
        "sekf,efd->sekd", hidden_act, down_weights, preferred_element_type=jnp.float32
    )
    half_sum = lax.psum_scatter(
        partial_out.astype(jnp.bfloat16), "tp", scatter_dimension=3, tiled=True
    )
    sent_back = lax.all_to_all(half_sum, "ep", split_axis=0, concat_axis=0, tiled=True)
    share_width = sent_back.shape[-1]
    picked = jnp.dot(
        dispatch_map,
        sent_back.reshape(experts * capacity, share_width),
        preferred_element_type=jnp.float32,
    )
    route_weight = expert_scores / jnp.sum(expert_scores, axis=-1, keepdims=True)
    expert_mix = jnp.sum(
        picked.reshape(rows_here, TOP_K, share_width) * route_weight[:, :, None], axis=1
    )
    own_part = lax.dynamic_slice_in_dim(
        residual, lax.axis_index("tp") * share_width, share_width, 1
    )
    updated = lax.all_gather((own_part + expert_mix).astype(jnp.bfloat16), "tp", axis=1, tiled=True)
    return updated


MESH = pl.DeviceIdType.MESH


def rest_body(n, att_ref, hid_ref, gain_ref, mix_ref, ow_hbm, gate_hbm, up_hbm, down_hbm, out_ref,
              heads, ow, gate, up, down, part, part_in, proj, mixed, resid, rows, act, eout, back, sums, mix, upd,
              send, recv, pair_send, pair_recv, local):
    me, tp = lax.axis_index("ep"), lax.axis_index("tp")
    seqs, width = hid_ref.shape
    half = width // 2
    feats = ow.shape[0]
    cols = att_ref.shape[1]
    inner = math.isqrt(n)
    outer = n // inner
    line, spot = me // inner, lax.rem(me, inner)

    def there(dl, ds):
        return lax.rem(line + dl + outer, outer) * inner + lax.rem(spot + ds + inner, inner)

    peers = [lax.rem(me + k, n) for k in range(1, n)]

    def mine(i):
        return pl.ds(pl.multiple_of(i * seqs, seqs), seqs)

    my_half = pl.ds(pl.multiple_of(tp * half, half), half)
    other_half = pl.ds(pl.multiple_of((1 - tp) * half, half), half)

    def remote(src, dst, s, r, ep, core):
        return pltpu.make_async_remote_copy(
            src_ref=src, dst_ref=dst, send_sem=s, recv_sem=r, device_id=(ep, core), device_id_type=MESH)

    loads = [
        pltpu.make_async_copy(ow_hbm.at[:, pl.ds(pl.multiple_of(tp * cols, cols), cols)], ow, local.at[0]),
        pltpu.make_async_copy(gate_hbm, gate, local.at[1]),
        pltpu.make_async_copy(up_hbm, up, local.at[2]),
        pltpu.make_async_copy(down_hbm.at[:, my_half], down.at[tp], local.at[3]),
    ]
    for c in loads:
        c.start()
    barrier = pltpu.get_barrier_semaphore()
    for p in peers:
        pl.semaphore_signal(barrier, inc=1, device_id=(p, tp), device_id_type=MESH)
    pl.semaphore_signal(barrier, inc=1, device_id=(me, 1 - tp), device_id_type=MESH)
    pl.semaphore_wait(barrier, n)

    sent = []

    def begin(c):
        c.start()
        sent.append(c)
        return c

    def gather(own, view, phase, use):
        far = {dl: begin(remote(own, view(me), send.at[phase, dl * inner], recv.at[phase, dl * inner],
                                there(dl, 0), tp)) for dl in range(1, outer)}
        near = []
        for dl in range(outer):
            source = there(-dl, 0)
            if dl:
                far[dl].wait_recv()
            block = view(source) if dl else own
            for ds in range(1, inner):
                near.append((there(-dl, -ds), begin(remote(
                    block, view(source), send.at[phase, dl * inner + ds], recv.at[phase, dl * inner + ds],
                    there(0, ds), tp))))
            if dl:
                use(dl * inner, source)
        for k, (source, c) in enumerate(near):
            c.wait_recv()
            use(k // (inner - 1) * inner + k % (inner - 1) + 1, source)

    swap_down = remote(down_hbm.at[:, other_half], down.at[tp], pair_send.at[0], pair_recv.at[0], me, 1 - tp)
    begin(swap_down)
    heads[mine(me), :] = att_ref[...]
    gather(att_ref, lambda s: heads.at[mine(s)], 0, lambda k, s: None)
    gains = [begin(remote(mix_ref.at[p], mix.at[me], send.at[5, k], recv.at[5, k], p, tp))
             for k, p in enumerate(peers)]
    mix[me] = mix_ref[me]
    loads[0].wait()
    part[...] = lax.dot_general(heads[...], ow[...], (((1,), (1,)), ((), ())), preferred_element_type=jnp.float32)
    swap = begin(remote(part, part_in, pair_send.at[1], pair_recv.at[1], me, 1 - tp))
    swap.wait_recv()
    proj[...] = (part[...] + part_in[...]).astype(jnp.bfloat16)
    my_feats = pl.ds(pl.multiple_of(me * feats, feats), feats)
    second = [begin(remote(proj.at[mine(p)], mixed.at[:, my_feats], send.at[1, k], recv.at[1, k], p, tp))
              for k, p in enumerate(peers)]
    mixed[:, my_feats] = proj[mine(me), :]
    for c in second:
        c.wait_recv()
    residual = hid_ref[...].astype(jnp.float32) + mixed[...].astype(jnp.float32)
    resid[...] = residual
    rows[mine(me), :] = root_norm(residual, gain_ref[...]).astype(jnp.bfloat16)

    fourth = []

    def pass_on(k, s):
        fourth.append(begin(remote(rows.at[mine(s), my_half], rows.at[mine(s), my_half],
                                   send.at[3, k], recv.at[3, k], me, 1 - tp)))

    gather(rows.at[mine(me), my_half], lambda s: rows.at[mine(s), my_half], 2, pass_on)
    loads[1].wait()
    loads[2].wait()
    for c in fourth:
        c.wait_recv()
    gate_act = jnp.dot(rows[...], gate[...], preferred_element_type=jnp.float32)
    up_act = jnp.dot(rows[...], up[...], preferred_element_type=jnp.float32)
    act[tp] = (gate_act / (1.0 + jnp.exp(-gate_act)) * up_act).astype(jnp.bfloat16)
    swap = begin(remote(act.at[tp], act.at[tp], pair_send.at[2], pair_recv.at[2], me, 1 - tp))
    loads[3].wait()
    swap_down.wait_recv()
    swap.wait_recv()
    for c in gains:
        c.wait_recv()
    eout[...] = ((jnp.dot(act[0], down[0], preferred_element_type=jnp.float32)
                  + jnp.dot(act[1], down[1], preferred_element_type=jnp.float32))
                 * mix[...].reshape(n * seqs, mix.shape[2])[:, :1]).astype(jnp.bfloat16)
    near = {}
    for dl in [d for d in range(1, outer)] + [0]:
        for ds in range(1, inner):
            k = dl * inner + ds
            near[k] = begin(remote(eout.at[mine(there(dl, ds))], back.at[k], send.at[4, k], recv.at[4, k],
                                   there(0, ds), tp))
    far = []
    for dl in [d for d in range(1, outer)] + [0]:
        summed = eout[mine(there(dl, 0)), :].astype(jnp.float32)
        for ds in range(1, inner):
            near[dl * inner + ds].wait_recv()
            summed = summed + back[dl * inner + ds].astype(jnp.float32)
        if dl:
            sums[dl] = summed.astype(jnp.bfloat16)
            far.append((dl, begin(remote(sums.at[dl], back.at[dl * inner], send.at[4, dl * inner],
                                         recv.at[4, dl * inner], there(dl, 0), tp))))
    for dl, c in far:
        c.wait_recv()
        summed = summed + back[dl * inner].astype(jnp.float32)
    total = resid[:, my_half]
    upd[:, my_half] = (total + summed).astype(jnp.bfloat16)
    swap = begin(remote(upd.at[:, my_half], upd.at[:, my_half], pair_send.at[3], pair_recv.at[3], me, 1 - tp))
    swap.wait_recv()
    out_ref[...] = upd[...]
    for c in sent:
        c.wait_send()


def rest_kernel(attended, hidden, out_weight, ffn_gain, expert_ids, expert_scores,
                gate_weights, up_weights, down_weights):
    n = lax.axis_size("ep")
    seqs, width = hidden.shape
    cols = attended.shape[1]
    feats = out_weight.shape[0]
    units = gate_weights.shape[2]
    half = width // 2
    route_weight = expert_scores / jnp.sum(expert_scores, axis=-1, keepdims=True)
    chosen = expert_ids[None, :, :] == jnp.arange(n, dtype=jnp.int32)[:, None, None]
    mix = jnp.sum(jnp.where(chosen, route_weight[None, :, :], 0.0), axis=-1, keepdims=True)
    mix = jnp.broadcast_to(mix, (n, seqs, 128))
    bf16, f32 = jnp.bfloat16, jnp.float32
    vmem = pl.BlockSpec(memory_space=pltpu.VMEM)
    hbm = pl.BlockSpec(memory_space=pl.ANY)
    return pl.pallas_call(
        functools.partial(rest_body, n),
        out_shape=jax.ShapeDtypeStruct((seqs, width), bf16),
        in_specs=[vmem] * 4 + [hbm] * 4,
        out_specs=vmem,
        scratch_shapes=[
            pltpu.VMEM((n * seqs, cols), bf16),
            pltpu.VMEM((feats, cols), bf16),
            pltpu.VMEM((width, units), bf16),
            pltpu.VMEM((width, units), bf16),
            pltpu.VMEM((2, units, half), bf16),
            pltpu.VMEM((n * seqs, feats), f32),
            pltpu.VMEM((n * seqs, feats), f32),
            pltpu.VMEM((n * seqs, feats), bf16),
            pltpu.VMEM((seqs, width), bf16),
            pltpu.VMEM((seqs, width), f32),
            pltpu.VMEM((n * seqs, width), bf16),
            pltpu.VMEM((2, n * seqs, units), bf16),
            pltpu.VMEM((n * seqs, half), bf16),
            pltpu.VMEM((n, seqs, half), bf16),
            pltpu.VMEM((math.isqrt(n), seqs, half), bf16),
            pltpu.VMEM((n, seqs, 128), f32),
            pltpu.VMEM((seqs, width), bf16),
            pltpu.SemaphoreType.DMA((6, n)),
            pltpu.SemaphoreType.DMA((6, n)),
            pltpu.SemaphoreType.DMA((4,)),
            pltpu.SemaphoreType.DMA((4,)),
            pltpu.SemaphoreType.DMA((4,)),
        ],
        compiler_params=pltpu.CompilerParams(
            collective_id=0, has_side_effects=True, vmem_limit_bytes=60 * 1024 * 1024),
    )(attended, hidden, ffn_gain[None, :], mix, out_weight, gate_weights[0], up_weights[0], down_weights[0])


def per_device(
    hidden,
    attn_gain,
    query_weight,
    key_weight,
    value_weight,
    forget_weight,
    forget_bias,
    cache_keys,
    cache_values,
    cache_logsum,
    lengths,
    out_weight,
    ffn_gain,
    expert_ids,
    expert_scores,
    gate_weights,
    up_weights,
    down_weights,
):
    attended, key_new, value_new, new_logsum = attend(
        hidden, attn_gain, query_weight, key_weight, value_weight, forget_weight, forget_bias,
        cache_keys, cache_values, cache_logsum, lengths)
    n = lax.axis_size("ep")
    square = math.isqrt(n) ** 2 == n
    rest = rest_kernel if out_weight.shape[0] % 128 == 0 and gate_weights.shape[0] == 1 and square else rest_general
    updated = rest(attended, hidden, out_weight, ffn_gain, expert_ids, expert_scores,
                   gate_weights, up_weights, down_weights)
    return (updated, key_new, value_new, new_logsum)


def solution(mesh):
    in_specs = (
        P("ep", None),
        P(),
        P(None, "tp"),
        P(None, "tp"),
        P(None, "tp"),
        P(None, "tp"),
        P("tp"),
        P("ep", "tp", None, None),
        P("ep", "tp", None, None),
        P("ep", "tp", None),
        P("ep"),
        P("ep", None),
        P(),
        P("ep", None),
        P("ep", None),
        P("ep", None, "tp"),
        P("ep", None, "tp"),
        P("ep", "tp", None),
    )
    out_specs = (P("ep", None), P("ep", "tp", None), P("ep", "tp", None), P("ep", "tp"))
    return jax.shard_map(
        per_device, mesh=mesh, in_specs=in_specs, out_specs=out_specs, check_vma=False
    )
```

```python
import functools
import math

import jax
import jax.numpy as jnp
from jax import lax
from jax.experimental import pallas as pl
from jax.experimental.pallas import tpu as pltpu
from jax.sharding import PartitionSpec as P

HD = 64
TOP_K = 6


epsilon = 1e-06


def root_norm(values_in, gain):
    floats = values_in.astype(jnp.float32)
    inv_root = lax.rsqrt(jnp.mean(floats * floats, axis=-1, keepdims=True) + epsilon)
    return floats * inv_root * gain.astype(jnp.float32)


def attend(hidden, attn_gain, query_weight, key_weight, value_weight, forget_weight, forget_bias,
           cache_keys, cache_values, cache_logsum, lengths):
    rows_here = hidden.shape[0]
    query_heads = query_weight.shape[1] // HD
    key_heads = key_weight.shape[1] // HD
    group_size = query_heads // key_heads
    cache_len = cache_keys.shape[-1]
    score_scale = HD ** (-0.5)
    normed = root_norm(hidden, attn_gain).astype(jnp.bfloat16)
    queries = jnp.dot(normed, query_weight, preferred_element_type=jnp.float32).astype(jnp.bfloat16)
    key_new = (
        jnp.dot(normed, key_weight, preferred_element_type=jnp.float32)
        .astype(jnp.bfloat16)
        .reshape(rows_here, key_heads, HD)
    )
    value_new = (
        jnp.dot(normed, value_weight, preferred_element_type=jnp.float32)
        .astype(jnp.bfloat16)
        .reshape(rows_here, key_heads, HD)
    )
    log_forget = jax.nn.log_sigmoid(
        jnp.dot(normed, forget_weight, preferred_element_type=jnp.float32) + forget_bias
    )
    positions = jnp.arange(cache_len, dtype=jnp.int32)
    is_last = positions[None, :] == (lengths - 1)[:, None]
    new_logsum = jnp.sum(jnp.where(is_last[:, None, :], cache_logsum, 0.0), axis=-1) + log_forget
    grouped = queries.reshape(rows_here, key_heads, group_size, HD)
    scores = jnp.einsum("sgjd,sgdp->sgjp", grouped, cache_keys, preferred_element_type=jnp.float32)
    scores = scores.reshape(rows_here, query_heads, cache_len) * score_scale
    scores = scores + new_logsum[:, :, None] - cache_logsum
    is_live = positions[None, :] < lengths[:, None]
    scores = jnp.where(is_live[:, None, :], scores, -jnp.inf)
    own_score = (
        jnp.einsum("sgjd,sgd->sgj", grouped, key_new, preferred_element_type=jnp.float32).reshape(
            rows_here, query_heads
        )
        * score_scale
    )
    top_score = jnp.maximum(jnp.max(scores, axis=-1), own_score)
    past_exp = jnp.exp(scores - top_score[:, :, None])
    own_exp = jnp.exp(own_score - top_score)
    denominator = jnp.sum(past_exp, axis=-1) + own_exp
    past_weight = (past_exp / denominator[:, :, None]).astype(jnp.bfloat16)
    own_weight = (own_exp / denominator).astype(jnp.bfloat16)
    attended = jnp.einsum(
        "sgjp,sgdp->sgjd",
        past_weight.reshape(rows_here, key_heads, group_size, cache_len),
        cache_values,
        preferred_element_type=jnp.float32,
    )
    attended = (
        attended
        + own_weight.astype(jnp.float32).reshape(rows_here, key_heads, group_size)[:, :, :, None]
        * value_new.astype(jnp.float32)[:, :, None, :]
    )
    attended = attended.reshape(rows_here, query_heads * HD).astype(jnp.bfloat16)
    return attended, key_new, value_new, new_logsum


def rest_general(attended, hidden, out_weight, ffn_gain, expert_ids, expert_scores,
                 gate_weights, up_weights, down_weights):
    rows_here = hidden.shape[0]
    whole_heads = lax.all_gather(attended, "tp", axis=1, tiled=True)
    projected = lax.dot_general(
        lax.all_gather(whole_heads, "ep", axis=0, tiled=True),
        out_weight,
        (((1,), (1,)), ((), ())),
        preferred_element_type=jnp.float32,
    ).astype(jnp.bfloat16)
    mixed = lax.all_to_all(projected, "ep", split_axis=0, concat_axis=1, tiled=True)
    residual = hidden.astype(jnp.float32) + mixed.astype(jnp.float32)
    ffn_in = root_norm(residual, ffn_gain).astype(jnp.bfloat16)
    ep_size = lax.axis_size("ep")
    local_experts = gate_weights.shape[0]
    experts = ep_size * local_experts
    route_count = rows_here * TOP_K
    capacity = 2 * ((route_count + experts - 1) // experts)
    flat_ids = expert_ids.reshape(route_count)
    onehot = (flat_ids[:, None] == jnp.arange(experts, dtype=jnp.int32)[None, :]).astype(jnp.int32)
    running = jnp.cumsum(onehot, axis=0)
    slot_index = jnp.sum(running * onehot, axis=1) - 1
    target = flat_ids * capacity + slot_index
    dispatch_map = (
        target[:, None] == jnp.arange(experts * capacity, dtype=jnp.int32)[None, :]
    ).astype(jnp.bfloat16)
    route_rows = jnp.repeat(ffn_in, TOP_K, axis=0)
    outgoing = lax.dot_general(
        dispatch_map, route_rows, (((0,), (0,)), ((), ())), preferred_element_type=jnp.float32
    )
    outgoing = outgoing.astype(jnp.bfloat16).reshape(
        ep_size, local_experts, capacity, ffn_in.shape[1]
    )
    arrived = lax.all_to_all(outgoing, "ep", split_axis=0, concat_axis=0, tiled=True)
    gate_act = jnp.einsum(
        "sekd,edf->sekf", arrived, gate_weights, preferred_element_type=jnp.float32
    )
    up_act = jnp.einsum("sekd,edf->sekf", arrived, up_weights, preferred_element_type=jnp.float32)
    hidden_act = (jax.nn.silu(gate_act) * up_act).astype(jnp.bfloat16)
    partial_out = jnp.einsum(
        "sekf,efd->sekd", hidden_act, down_weights, preferred_element_type=jnp.float32
    )
    half_sum = lax.psum_scatter(
        partial_out.astype(jnp.bfloat16), "tp", scatter_dimension=3, tiled=True
    )
    sent_back = lax.all_to_all(half_sum, "ep", split_axis=0, concat_axis=0, tiled=True)
    share_width = sent_back.shape[-1]
    picked = jnp.dot(
        dispatch_map,
        sent_back.reshape(experts * capacity, share_width),
        preferred_element_type=jnp.float32,
    )
    route_weight = expert_scores / jnp.sum(expert_scores, axis=-1, keepdims=True)
    expert_mix = jnp.sum(
        picked.reshape(rows_here, TOP_K, share_width) * route_weight[:, :, None], axis=1
    )
    own_part = lax.dynamic_slice_in_dim(
        residual, lax.axis_index("tp") * share_width, share_width, 1
    )
    updated = lax.all_gather((own_part + expert_mix).astype(jnp.bfloat16), "tp", axis=1, tiled=True)
    return updated


MESH = pl.DeviceIdType.MESH


def rest_body(n, att_ref, hid_ref, gain_ref, mix_ref, ow_hbm, gate_hbm, up_hbm, down_hbm, out_ref,
              heads, ow, gate, up, down, part, part_in, proj, mixed, resid, rows, act, eout, back, sums, mix, upd,
              send, recv, pair_send, pair_recv, local):
    me, tp = lax.axis_index("ep"), lax.axis_index("tp")
    seqs, width = hid_ref.shape
    half = width // 2
    feats = ow.shape[0]
    cols = att_ref.shape[1]
    inner = math.isqrt(n)
    outer = n // inner
    line, spot = me // inner, lax.rem(me, inner)

    def there(dl, ds):
        return lax.rem(line + dl + outer, outer) * inner + lax.rem(spot + ds + inner, inner)

    peers = [lax.rem(me + k, n) for k in range(1, n)]

    def mine(i):
        return pl.ds(pl.multiple_of(i * seqs, seqs), seqs)

    my_half = pl.ds(pl.multiple_of(tp * half, half), half)
    other_half = pl.ds(pl.multiple_of((1 - tp) * half, half), half)

    def remote(src, dst, s, r, ep, core):
        return pltpu.make_async_remote_copy(
            src_ref=src, dst_ref=dst, send_sem=s, recv_sem=r, device_id=(ep, core), device_id_type=MESH)

    loads = [
        pltpu.make_async_copy(ow_hbm.at[:, pl.ds(pl.multiple_of(tp * cols, cols), cols)], ow, local.at[0]),
        pltpu.make_async_copy(gate_hbm, gate, local.at[1]),
        pltpu.make_async_copy(up_hbm, up, local.at[2]),
        pltpu.make_async_copy(down_hbm.at[:, my_half], down.at[tp], local.at[3]),
    ]
    for c in loads:
        c.start()
    barrier = pltpu.get_barrier_semaphore()
    for p in peers:
        pl.semaphore_signal(barrier, inc=1, device_id=(p, tp), device_id_type=MESH)
    pl.semaphore_signal(barrier, inc=1, device_id=(me, 1 - tp), device_id_type=MESH)
    pl.semaphore_wait(barrier, n)

    sent = []

    def begin(c):
        c.start()
        sent.append(c)
        return c

    def gather(own, view, phase, use):
        far = {dl: begin(remote(own, view(me), send.at[phase, dl * inner], recv.at[phase, dl * inner],
                                there(dl, 0), tp)) for dl in range(1, outer)}
        near = [[] for _ in range(outer)]
        for dl in range(outer):
            source = there(-dl, 0)
            if dl:
                far[dl].wait_recv()
            block = view(source) if dl else own
            for ds in range(1, inner):
                near[dl].append((dl * inner + ds, there(-dl, -ds), begin(remote(
                    block, view(source), send.at[phase, dl * inner + ds], recv.at[phase, dl * inner + ds],
                    there(0, ds), tp))))
            if dl:
                use(dl * inner, source)
        return near

    swap_down = remote(down_hbm.at[:, other_half], down.at[tp], pair_send.at[0], pair_recv.at[0], me, 1 - tp)
    begin(swap_down)
    heads[mine(me), :] = att_ref[...]
    arriving = gather(att_ref, lambda s: heads.at[mine(s)], 0, lambda k, s: None)
    gains = [begin(remote(mix_ref.at[p], mix.at[me], send.at[5, k], recv.at[5, k], p, tp))
             for k, p in enumerate(peers)]
    mix[me] = mix_ref[me]
    loads[0].wait()
    for group in arriving:
        for _, _, c in group:
            c.wait_recv()
    part[...] = lax.dot_general(heads[...], ow[...], (((1,), (1,)), ((), ())), preferred_element_type=jnp.float32)
    swap = begin(remote(part, part_in, pair_send.at[1], pair_recv.at[1], me, 1 - tp))
    swap.wait_recv()
    proj[...] = (part[...] + part_in[...]).astype(jnp.bfloat16)
    my_feats = pl.ds(pl.multiple_of(me * feats, feats), feats)
    second = [begin(remote(proj.at[mine(p)], mixed.at[:, my_feats], send.at[1, k], recv.at[1, k], p, tp))
              for k, p in enumerate(peers)]
    mixed[:, my_feats] = proj[mine(me), :]
    for c in second:
        c.wait_recv()
    residual = hid_ref[...].astype(jnp.float32) + mixed[...].astype(jnp.float32)
    resid[...] = residual
    rows[mine(me), :] = root_norm(residual, gain_ref[...]).astype(jnp.bfloat16)

    fourth = [[] for _ in range(outer)]

    def pass_on(k, s):
        fourth[k // inner].append(begin(remote(rows.at[mine(s), my_half], rows.at[mine(s), my_half],
                                   send.at[3, k], recv.at[3, k], me, 1 - tp)))

    arriving = gather(rows.at[mine(me), my_half], lambda s: rows.at[mine(s), my_half], 2, pass_on)
    near, swaps = {}, {}

    def some(dl):
        size = inner * seqs
        return pl.ds(pl.multiple_of(lax.rem(line - dl + outer, outer) * size, size), size)

    for step in range(outer + 2):
        if step < outer:
            for k, source, c in arriving[step]:
                c.wait_recv()
                pass_on(k, source)
        if step == 0:
            loads[1].wait()
            loads[2].wait()
            loads[3].wait()
            swap_down.wait_recv()
            for c in gains:
                c.wait_recv()
        dl = step - 1
        if 0 <= dl < outer:
            for c in fourth[dl]:
                c.wait_recv()
            block = rows[some(dl), :]
            gate_act = jnp.dot(block, gate[...], preferred_element_type=jnp.float32)
            up_act = jnp.dot(block, up[...], preferred_element_type=jnp.float32)
            act[tp, some(dl), :] = (gate_act / (1.0 + jnp.exp(-gate_act)) * up_act).astype(jnp.bfloat16)
            swaps[dl] = begin(remote(act.at[tp, some(dl)], act.at[tp, some(dl)],
                                     pair_send.at[4 + dl], pair_recv.at[4 + dl], me, 1 - tp))
        dl = step - 2
        if dl >= 0:
            swaps[dl].wait_recv()
            weight = mix[pl.ds(lax.rem(line - dl + outer, outer) * inner, inner)]
            eout[some(dl), :] = ((jnp.dot(act[0, some(dl), :], down[0], preferred_element_type=jnp.float32)
                                  + jnp.dot(act[1, some(dl), :], down[1], preferred_element_type=jnp.float32))
                                 * weight.reshape(inner * seqs, mix.shape[2])[:, :1]).astype(jnp.bfloat16)
            to = (outer - dl) % outer
            for ds in range(1, inner):
                k = to * inner + ds
                near[k] = begin(remote(eout.at[mine(there(to, ds))], back.at[k], send.at[4, k], recv.at[4, k],
                                       there(0, ds), tp))
    far = []
    for dl in [d for d in range(outer - 1, -1, -1)]:
        summed = eout[mine(there(dl, 0)), :].astype(jnp.float32)
        for ds in range(1, inner):
            near[dl * inner + ds].wait_recv()
            summed = summed + back[dl * inner + ds].astype(jnp.float32)
        if dl:
            sums[dl] = summed.astype(jnp.bfloat16)
            far.append((dl, begin(remote(sums.at[dl], back.at[dl * inner], send.at[4, dl * inner],
                                         recv.at[4, dl * inner], there(dl, 0), tp))))
    for dl, c in far:
        c.wait_recv()
        summed = summed + back[dl * inner].astype(jnp.float32)
    total = resid[:, my_half]
    upd[:, my_half] = (total + summed).astype(jnp.bfloat16)
    swap = begin(remote(upd.at[:, my_half], upd.at[:, my_half], pair_send.at[3], pair_recv.at[3], me, 1 - tp))
    swap.wait_recv()
    out_ref[...] = upd[...]
    for c in sent:
        c.wait_send()


def rest_kernel(attended, hidden, out_weight, ffn_gain, expert_ids, expert_scores,
                gate_weights, up_weights, down_weights):
    n = lax.axis_size("ep")
    seqs, width = hidden.shape
    cols = attended.shape[1]
    feats = out_weight.shape[0]
    units = gate_weights.shape[2]
    half = width // 2
    route_weight = expert_scores / jnp.sum(expert_scores, axis=-1, keepdims=True)
    chosen = expert_ids[None, :, :] == jnp.arange(n, dtype=jnp.int32)[:, None, None]
    mix = jnp.sum(jnp.where(chosen, route_weight[None, :, :], 0.0), axis=-1, keepdims=True)
    mix = jnp.broadcast_to(mix, (n, seqs, 128))
    bf16, f32 = jnp.bfloat16, jnp.float32
    vmem = pl.BlockSpec(memory_space=pltpu.VMEM)
    hbm = pl.BlockSpec(memory_space=pl.ANY)
    return pl.pallas_call(
        functools.partial(rest_body, n),
        out_shape=jax.ShapeDtypeStruct((seqs, width), bf16),
        in_specs=[vmem] * 4 + [hbm] * 4,
        out_specs=vmem,
        scratch_shapes=[
            pltpu.VMEM((n * seqs, cols), bf16),
            pltpu.VMEM((feats, cols), bf16),
            pltpu.VMEM((width, units), bf16),
            pltpu.VMEM((width, units), bf16),
            pltpu.VMEM((2, units, half), bf16),
            pltpu.VMEM((n * seqs, feats), f32),
            pltpu.VMEM((n * seqs, feats), f32),
            pltpu.VMEM((n * seqs, feats), bf16),
            pltpu.VMEM((seqs, width), bf16),
            pltpu.VMEM((seqs, width), f32),
            pltpu.VMEM((n * seqs, width), bf16),
            pltpu.VMEM((2, n * seqs, units), bf16),
            pltpu.VMEM((n * seqs, half), bf16),
            pltpu.VMEM((n, seqs, half), bf16),
            pltpu.VMEM((math.isqrt(n), seqs, half), bf16),
            pltpu.VMEM((n, seqs, 128), f32),
            pltpu.VMEM((seqs, width), bf16),
            pltpu.SemaphoreType.DMA((6, n)),
            pltpu.SemaphoreType.DMA((6, n)),
            pltpu.SemaphoreType.DMA((4 + math.isqrt(n),)),
            pltpu.SemaphoreType.DMA((4 + math.isqrt(n),)),
            pltpu.SemaphoreType.DMA((4,)),
        ],
        compiler_params=pltpu.CompilerParams(
            collective_id=0, has_side_effects=True, vmem_limit_bytes=60 * 1024 * 1024),
    )(attended, hidden, ffn_gain[None, :], mix, out_weight, gate_weights[0], up_weights[0], down_weights[0])


def per_device(
    hidden,
    attn_gain,
    query_weight,
    key_weight,
    value_weight,
    forget_weight,
    forget_bias,
    cache_keys,
    cache_values,
    cache_logsum,
    lengths,
    out_weight,
    ffn_gain,
    expert_ids,
    expert_scores,
    gate_weights,
    up_weights,
    down_weights,
):
    attended, key_new, value_new, new_logsum = attend(
        hidden, attn_gain, query_weight, key_weight, value_weight, forget_weight, forget_bias,
        cache_keys, cache_values, cache_logsum, lengths)
    n = lax.axis_size("ep")
    square = math.isqrt(n) ** 2 == n
    rest = rest_kernel if out_weight.shape[0] % 128 == 0 and gate_weights.shape[0] == 1 and square else rest_general
    updated = rest(attended, hidden, out_weight, ffn_gain, expert_ids, expert_scores,
                   gate_weights, up_weights, down_weights)
    return (updated, key_new, value_new, new_logsum)


def solution(mesh):
    in_specs = (
        P("ep", None),
        P(),
        P(None, "tp"),
        P(None, "tp"),
        P(None, "tp"),
        P(None, "tp"),
        P("tp"),
        P("ep", "tp", None, None),
        P("ep", "tp", None, None),
        P("ep", "tp", None),
        P("ep"),
        P("ep", None),
        P(),
        P("ep", None),
        P("ep", None),
        P("ep", None, "tp"),
        P("ep", None, "tp"),
        P("ep", "tp", None),
    )
    out_specs = (P("ep", None), P("ep", "tp", None), P("ep", "tp", None), P("ep", "tp"))
    return jax.shard_map(
        per_device, mesh=mesh, in_specs=in_specs, out_specs=out_specs, check_vma=False
    )
```
